32 devices in a mesh: fs: 8 (over z, y), tp: 4 (over x, core).
Axes of the slice: x: 2, y: 2, z: 4, core: 2. Of those that a mesh axis runs over, the one named last changes fastest.
Arguments:
- stream: bfloat16 [3072, 2048], P('fs', 'tp'), may hold values from -3 to 3
- gain_first: float32 [2048], replicated, may hold values from 0.1 to 1.9
- gain_mixer: float32 [2048], replicated, may hold values from 0.1 to 1.9
- gain_second: float32 [2048], replicated, may hold values from 0.1 to 1.9
- gate_weight: float32 [2048, 5632], P('fs', 'tp'), may hold values from -0.125 to 0.125
- gate_scale: float32 [5632], P('tp'), may hold values from 0.5 to 2
- up_weight: float32 [2048, 5632], P('fs', 'tp'), may hold values from -0.125 to 0.125
- up_scale: float32 [5632], P('tp'), may hold values from 0.5 to 2
- down_weight: float32 [5632, 2048], P('tp', 'fs'), may hold values from -0.109375 to 0.109375
- down_scale: float32 [2048], P('tp'), may hold values from 0.5 to 2
- pool_in_weight: float32 [2048, 512], P('fs', 'tp'), may hold values from -0.125 to 0.125
- pool_in_scale: float32 [512], P('tp'), may hold values from 0.5 to 2
- pool_out_weight: float32 [512, 2048], P('tp', 'fs'), may hold values from -0.375 to 0.375
- pool_out_scale: float32 [2048], P('tp'), may hold values from 0.5 to 2
Outputs:
- layer_out: bfloat16 [3072, 2048], P('fs', 'tp')
The draws below stay inside these ranges and needn't reach their ends.
All inputs are finite; a program needn't handle non-finite values.
Results may differ from the reference program's by a relative error of at most 0.025.
Values may be sent and summed in bfloat16 or wider, within the bound.
No kernel may reach another device: no remote copies, remote signals or barrier semaphores. Data moves between devices by JAX's collectives and lax.ppermute only.
A program may use at most 64 MiB of HBM per device.

```python
import math
import jax
import jax.numpy as jnp
from jax import lax

D = 2048
FF = 5632
P_SIZE = 512
SEQ = 128
TOKENS = 3072
N_TP = 4


def strengthened(drawn, rng, source, target, blocks, factor):
    owner, partner = [(jnp.arange(drawn.shape[dim]) // (drawn.shape[dim] // blocks)).reshape([-1 if axis == dim else 1 for axis in range(drawn.ndim)]) for dim in (source, target)]
    chosen = jax.random.permutation(rng, blocks)[partner]
    strong = (owner == chosen) | (owner == (partner + blocks // 2) % blocks)
    return jnp.where(strong, factor * drawn, drawn)


def level_of(stream_key, extent, cuts, least, top_value):
    level, own = 1.0, jax.random.fold_in(stream_key, 6)
    for axis_at, blocks in cuts:
        steps = jnp.exp(jax.random.uniform(jax.random.fold_in(own, axis_at), (blocks,), jnp.float32, least / len(cuts), top_value / len(cuts)))
        level = level * jnp.repeat(steps, extent[axis_at] // blocks).reshape([-1 if axis == axis_at else 1 for axis in range(len(extent))])
    return level


def normal_values(own_key, extent, scale, limit, cuts=(), kind=jnp.bfloat16):
    values = jax.random.normal(own_key, extent, jnp.float32) * scale
    if len(cuts) > 0:
        values = level_of(own_key, extent, cuts, -0.22, 0.18) * values
    return jnp.clip(values, min=-limit, max=limit).astype(kind)


def heavy_noise(key, shape, width, bound, pieces, heavy, dtype=jnp.bfloat16):
    result = width * jax.random.normal(key, shape, jnp.float32)
    if pieces:
        result = result * level_of(key, shape, pieces, -0.22, 0.18)
    return jnp.clip(strengthened(result, jax.random.fold_in(key, 3), *heavy), -bound, bound).astype(dtype)


def setup_inputs(seed: int = 0) -> dict:
    streams_of = jax.random.split(jax.random.key(seed), 15)
    return {
        "stream": normal_values(streams_of[0], (TOKENS, D), 0.5, 3.0, ((0, 8), (1, 4))),
        "gain_first": jnp.clip(1.0 + 0.18 * jax.random.normal(streams_of[1], (D,), jnp.float32), 0.1, 1.9),
        "gain_mixer": jnp.clip(1.0 + 0.18 * jax.random.normal(streams_of[2], (D,), jnp.float32), 0.1, 1.9),
        "gain_second": jnp.clip(1.0 + 0.18 * jax.random.normal(streams_of[3], (D,), jnp.float32), 0.1, 1.9),
        "gate_weight": normal_values(streams_of[4], (D, FF), D ** -0.5, 0.125, ((0, 8), (1, 4)), jnp.float32),
        "gate_scale": jnp.clip(jnp.exp(math.log(2.0) - 1.3862944 * jax.random.uniform(streams_of[5], (FF,), jnp.float32) ** level_of(streams_of[5], (FF,), ((0, 4),), -0.2, 0.2)), 0.5, 2.0),
        "up_weight": normal_values(streams_of[6], (D, FF), D ** -0.5, 0.125, ((0, 8), (1, 4)), jnp.float32),
        "up_scale": jnp.clip(jnp.exp(math.log(2.0) - 1.3862944 * jax.random.uniform(streams_of[7], (FF,), jnp.float32) ** level_of(streams_of[7], (FF,), ((0, 4),), -0.2, 0.2)), 0.5, 2.0),
        "down_weight": heavy_noise(streams_of[8], (FF, D), FF ** -0.5, 0.109375, ((0, 4), (1, 8)), (0, 1, 8, 2.0), jnp.float32),
        "down_scale": jnp.clip(jnp.exp(math.log(2.0) - 1.3862944 * jax.random.uniform(streams_of[9], (D,), jnp.float32) ** level_of(streams_of[9], (D,), ((0, 4),), -0.2, 0.2)), 0.5, 2.0),
        "pool_in_weight": normal_values(streams_of[10], (D, P_SIZE), D ** -0.5, 0.125, ((0, 8), (1, 4)), jnp.float32),
        "pool_in_scale": jnp.clip(jnp.exp(math.log(2.0) - 1.3862944 * jax.random.uniform(streams_of[11], (P_SIZE,), jnp.float32) ** level_of(streams_of[11], (P_SIZE,), ((0, 4),), -0.2, 0.2)), 0.5, 2.0),
        "pool_out_weight": heavy_noise(streams_of[12], (P_SIZE, D), P_SIZE ** -0.5, 0.375, ((0, 4), (1, 8)), (0, 1, 8, 2.0), jnp.float32),
        "pool_out_scale": jnp.clip(jnp.exp(math.log(2.0) - 1.3862944 * jax.random.uniform(streams_of[13], (D,), jnp.float32) ** level_of(streams_of[13], (D,), ((0, 4),), -0.2, 0.2)), 0.5, 2.0),
    }


eps = 1e-06
WINDOWS = (2, 4, 8, 16)

def rms_norm(values, norm_gain):
    floats = values.astype(jnp.float32)
    scaled = floats * lax.rsqrt(lax.optimization_barrier(jnp.mean(floats * floats, axis=-1, keepdims=True)) + eps)
    return (scaled * norm_gain).astype(jnp.bfloat16)

def block_sum(left_rows, right_rows, column_scale):
    block_rows = right_rows.shape[0] // N_TP
    running = jnp.zeros((left_rows.shape[0], right_rows.shape[1]), jnp.float32)
    for blocks in range(N_TP):
        block_part = jnp.dot(left_rows[:, blocks * block_rows:(blocks + 1) * block_rows], right_rows[blocks * block_rows:(blocks + 1) * block_rows], preferred_element_type=jnp.float32).astype(jnp.bfloat16)
        block_part = lax.optimization_barrier(block_part)
        running = running + block_part.astype(jnp.float32)
    return running * column_scale

def feed_forward(normed, gate_half, gate_scale, up_half, up_scale, down_half, down_scale):
    gate_sum = jnp.dot(normed, gate_half, preferred_element_type=jnp.float32) * gate_scale
    up_sum = jnp.dot(normed, up_half, preferred_element_type=jnp.float32) * up_scale
    hidden = (jax.nn.silu(gate_sum) * up_sum).astype(jnp.bfloat16)
    return block_sum(hidden, down_half, down_scale)

def pooling(pool_input):
    channels = pool_input.shape[1]
    floats = pool_input.astype(jnp.float32).reshape(-1, SEQ, channels)
    csum = jnp.concatenate([jnp.zeros((floats.shape[0], 1, channels), jnp.float32), jnp.cumsum(floats, axis=1)], axis=1)
    position = jnp.arange(SEQ)
    channel_group = jnp.arange(channels) * 4 // channels
    pooled = -floats
    for group_index, window in enumerate(WINDOWS):
        before = window // 2
        after_span = window - before
        upper_sum = jnp.pad(csum, ((0, 0), (0, after_span), (0, 0)), mode='edge')[:, after_span:after_span + SEQ]
        lower_sum = jnp.pad(csum, ((0, 0), (before, 0), (0, 0)), mode='edge')[:, :SEQ]
        counts = (jnp.minimum(position + after_span, SEQ) - jnp.maximum(position - before, 0)).astype(jnp.float32)
        window_mean = (upper_sum - lower_sum) / counts[None, :, None]
        select = (channel_group == group_index).astype(jnp.float32)
        pooled = pooled + window_mean * select
    return pooled.reshape(-1, channels).astype(jnp.bfloat16)

def reference(stream, gain_first, gain_mixer, gain_second, gate_weight, gate_scale, up_weight, up_scale, down_weight, down_scale, pool_in_weight, pool_in_scale, pool_out_weight, pool_out_scale):
    gate_half = gate_weight.astype(jnp.bfloat16)
    up_half = up_weight.astype(jnp.bfloat16)
    down_half = down_weight.astype(jnp.bfloat16)
    in_half = pool_in_weight.astype(jnp.bfloat16)
    out_half = pool_out_weight.astype(jnp.bfloat16)
    first_branch = feed_forward(rms_norm(stream, gain_first), gate_half, gate_scale, up_half, up_scale, down_half, down_scale)
    after_first = (stream.astype(jnp.float32) + 0.5 * first_branch).astype(jnp.bfloat16)
    mixer_normed = rms_norm(after_first, gain_mixer)
    pool_input = (jnp.dot(mixer_normed, in_half, preferred_element_type=jnp.float32) * pool_in_scale).astype(jnp.bfloat16)
    pooled = pooling(pool_input)
    after_mix = (after_first.astype(jnp.float32) + block_sum(pooled, out_half, pool_out_scale)).astype(jnp.bfloat16)
    second_branch = feed_forward(rms_norm(after_mix, gain_second), gate_half, gate_scale, up_half, up_scale, down_half, down_scale)
    return (after_mix.astype(jnp.float32) + 0.5 * second_branch).astype(jnp.bfloat16)
```

```python
import jax
import jax.numpy as jnp
from jax import lax
from jax.sharding import PartitionSpec as P

SEQ = 128


eps = 1e-06
WINDOWS = (2, 4, 8, 16)


def swap(value, axis, mask):
    count = lax.axis_size(axis)
    return lax.ppermute(value, axis, [(i, i ^ mask) for i in range(count)])


def power_of_two(count):
    return count & (count - 1) == 0


def spread(shard, axis):
    count = lax.axis_size("fs")
    got = {0: shard}
    for mask in range(2, count, 2):
        if mask & (mask - 1) == 0:
            got[mask] = swap(shard, "fs", mask)
    if count > 1:
        got[1] = swap(shard, "fs", 1)
    for mask in range(2, count, 2):
        if mask not in got:
            low = mask & -mask
            got[mask] = swap(got[mask ^ low], "fs", low)
    for mask in range(3, count, 2):
        if mask == 3:
            near, far = got[2], got[1]
            half = shard.shape[0] // 2
            got[3] = jnp.concatenate([swap(near[:half], "fs", 1), swap(far[half:], "fs", 2)], axis=0)
        else:
            got[mask] = swap(got[mask ^ 1], "fs", 1)
    return got


def gather_fs(shard, axis):
    count = lax.axis_size("fs")
    if not power_of_two(count):
        return lax.all_gather(shard, "fs", axis=axis, tiled=True)
    me = lax.axis_index("fs")
    got = spread(shard, axis)
    shape = list(shard.shape)
    width = shape[axis]
    shape[axis] = width * count
    whole = jnp.zeros(shape, shard.dtype)
    for mask, piece in got.items():
        start = [0, 0]
        start[axis] = (me ^ mask) * width
        whole = lax.dynamic_update_slice(whole, piece, start)
    return whole


def normed(own_columns, norm_gain):
    gathered = lax.all_gather(own_columns, "tp", axis=1, tiled=True)
    floats = gathered.astype(jnp.float32)
    scaled = floats * lax.rsqrt(jnp.mean(floats * floats, axis=-1, keepdims=True) + eps)
    return (scaled * norm_gain).astype(jnp.bfloat16)


def residual_add(own_columns, partial_value, column_scale, factor):
    summed = lax.psum_scatter(
        partial_value.astype(jnp.bfloat16), "tp", scatter_dimension=1, tiled=True
    ).astype(jnp.float32)
    return (own_columns.astype(jnp.float32) + factor * (summed * column_scale)).astype(jnp.bfloat16)


def pooling(pool_input):
    channels = pool_input.shape[1]
    floats = pool_input.astype(jnp.float32).reshape(-1, SEQ, channels)
    csum = jnp.concatenate(
        [jnp.zeros((floats.shape[0], 1, channels), jnp.float32), jnp.cumsum(floats, axis=1)], axis=1
    )
    position = jnp.arange(SEQ)
    channel_index = lax.axis_index("tp") * channels + jnp.arange(channels, dtype=jnp.int32)
    channel_group = channel_index * 4 // (channels * lax.axis_size("tp"))
    pooled = -floats
    for group_index, window in enumerate(WINDOWS):
        before = window // 2
        after_span = window - before
        upper_sum = jnp.pad(csum, ((0, 0), (0, after_span), (0, 0)), mode="edge")[
            :, after_span : after_span + SEQ
        ]
        lower_sum = jnp.pad(csum, ((0, 0), (before, 0), (0, 0)), mode="edge")[:, :SEQ]
        counts = (
            jnp.minimum(position + after_span, SEQ) - jnp.maximum(position - before, 0)
        ).astype(jnp.float32)
        window_mean = (upper_sum - lower_sum) / counts[None, :, None]
        select = (channel_group == group_index).astype(jnp.float32)
        pooled = pooled + window_mean * select
    return pooled.reshape(-1, channels).astype(jnp.bfloat16)


def body(
    stream,
    gain_first,
    gain_mixer,
    gain_second,
    gate_weight,
    gate_scale,
    up_weight,
    up_scale,
    down_weight,
    down_scale,
    pool_in_weight,
    pool_in_scale,
    pool_out_weight,
    pool_out_scale,
):
    hidden_width = gate_weight.shape[1]
    gate_in = jnp.concatenate([gate_weight, pool_in_weight], axis=1).astype(jnp.bfloat16)
    up_half = up_weight.astype(jnp.bfloat16)
    down_out = jnp.concatenate([down_weight, pool_out_weight], axis=0).astype(jnp.bfloat16)
    gate_in_whole = gather_fs(gate_in, 0)
    up_whole = gather_fs(up_half, 0)
    down_out_whole = gather_fs(down_out, 1)
    gate_whole, in_whole = gate_in_whole[:, :hidden_width], gate_in_whole[:, hidden_width:]
    down_whole, out_whole = down_out_whole[:hidden_width], down_out_whole[hidden_width:]

    def feed_forward(normed_rows):
        gate_sum = jnp.dot(normed_rows, gate_whole, preferred_element_type=jnp.float32) * gate_scale
        up_sum = jnp.dot(normed_rows, up_whole, preferred_element_type=jnp.float32) * up_scale
        hidden = (jax.nn.silu(gate_sum) * up_sum).astype(jnp.bfloat16)
        return jnp.dot(hidden, down_whole, preferred_element_type=jnp.float32)

    after_first = residual_add(stream, feed_forward(normed(stream, gain_first)), down_scale, 0.5)
    mixer_normed = normed(after_first, gain_mixer)
    pool_input = (
        jnp.dot(mixer_normed, in_whole, preferred_element_type=jnp.float32) * pool_in_scale
    ).astype(jnp.bfloat16)
    pooled = pooling(pool_input)
    tp_count = lax.axis_size("tp")
    all_pooled = lax.all_gather(pooled, "tp", axis=1, tiled=True)
    out_columns = lax.all_to_all(out_whole, "tp", split_axis=1, concat_axis=0, tiled=True)
    mixed = jnp.dot(all_pooled, out_columns, preferred_element_type=jnp.float32)
    after_mix = (after_first.astype(jnp.float32) + mixed * pool_out_scale).astype(jnp.bfloat16)
    return residual_add(after_mix, feed_forward(normed(after_mix, gain_second)), down_scale, 0.5)


def solution(mesh):
    placed = (
        P("fs", "tp"),
        P(),
        P(),
        P(),
        P("fs", "tp"),
        P("tp"),
        P("fs", "tp"),
        P("tp"),
        P("tp", "fs"),
        P("tp"),
        P("fs", "tp"),
        P("tp"),
        P("tp", "fs"),
        P("tp"),
    )
    return jax.shard_map(body, mesh=mesh, in_specs=placed, out_specs=P("fs", "tp"), check_vma=False)
```

```python
import jax
import jax.numpy as jnp
from jax import lax
from jax.experimental import pallas as pl
from jax.sharding import PartitionSpec as P

SEQ = 128


eps = 1e-06
WINDOWS = (2, 4, 8, 16)


def swap(value, axis, mask):
    count = lax.axis_size(axis)
    return lax.ppermute(value, axis, [(i, i ^ mask) for i in range(count)])


def spread(shard):
    count = lax.axis_size("fs")
    got = {0: shard}
    if count > 1:
        got[1] = swap(shard, "fs", 1)
    for mask in range(2, count, 2):
        if mask & (mask - 1) == 0:
            got[mask] = swap(shard, "fs", mask)
    for mask in range(2, count, 2):
        if mask not in got:
            low = mask & -mask
            got[mask] = swap(got[mask ^ low], "fs", low)
    for mask in range(3, count, 2):
        if mask == 3:
            near, far = got[2], got[1]
            half = shard.shape[0] // 2
            got[3] = (swap(near[:half], "fs", 1), swap(far[half:], "fs", 2))
        else:
            got[mask] = swap(got[mask ^ 1], "fs", 1)
    return got


def unfilled(shape, dtype):
    return pl.pallas_call(
        lambda ref: None,
        out_shape=jax.ShapeDtypeStruct(shape, dtype),
        out_specs=pl.BlockSpec(memory_space=pl.ANY),
        name="unfilled",
    )()


def gather_fs(shard, axis):
    count = lax.axis_size("fs")
    me = lax.axis_index("fs")
    got = spread(shard)
    shape = list(shard.shape)
    width = shape[axis]
    shape[axis] = width * count
    per_block = count // lax.axis_size("tp")
    me = me ^ (lax.axis_index("tp") * per_block)
    whole = unfilled(shape, shard.dtype)
    for mask, piece in got.items():
        place = (me ^ mask) * width
        parts = piece if isinstance(piece, tuple) else (piece,)
        row = 0
        for part in parts:
            start = [row, 0]
            start[axis] = start[axis] + place
            whole = lax.dynamic_update_slice(whole, part, start)
            row += part.shape[0]
    return whole


def relative_gain(gain):
    count = lax.axis_size("tp")
    block = gain.shape[0] // count
    me = lax.axis_index("tp")
    return jnp.concatenate([lax.dynamic_slice(gain, ((me ^ m) * block,), (block,)) for m in range(count)])


def spread_tp(own):
    count = lax.axis_size("tp")
    got = {0: own}
    for mask in range(2, count, 2):
        low = mask & -mask
        got[mask] = swap(got[mask ^ low], "tp", low)
    for mask in range(1, count, 2):
        got[mask] = swap(got[mask ^ 1], "tp", 1)
    return [got[m] for m in range(count)]


def normed(own_columns, gain_relative):
    blocks = spread_tp(own_columns)
    floats = [b.astype(jnp.float32) for b in blocks]
    total = sum(jnp.sum(f * f, axis=-1, keepdims=True) for f in floats)
    width = own_columns.shape[1]
    factor = lax.rsqrt(total / (width * len(blocks)) + eps)
    gains = [gain_relative[m * width : (m + 1) * width] for m in range(len(blocks))]
    return jnp.concatenate([(f * factor * g).astype(jnp.bfloat16) for f, g in zip(floats, gains)], axis=1)


def residual_add(own_columns, partial_value, column_scale, factor):
    count = lax.axis_size("tp")
    width = own_columns.shape[1]
    sums = [partial_value[:, m * width : (m + 1) * width] for m in range(count)]
    bit = 1
    while bit < count:
        keep = {}
        for m in range(count):
            if m % (2 * bit) == bit:
                arrived = swap(sums[m].astype(jnp.bfloat16), "tp", bit)
                keep[m ^ bit] = sums[m ^ bit].astype(jnp.float32) + arrived.astype(jnp.float32)
        for m, value in keep.items():
            sums[m] = value
        bit *= 2
    return (own_columns.astype(jnp.float32) + factor * (sums[0] * column_scale)).astype(jnp.bfloat16)


def pooling(pool_input):
    channels = pool_input.shape[1]
    floats = pool_input.astype(jnp.float32).reshape(-1, SEQ, channels)
    csum = jnp.concatenate(
        [jnp.zeros((floats.shape[0], 1, channels), jnp.float32), jnp.cumsum(floats, axis=1)], axis=1
    )
    position = jnp.arange(SEQ)
    channel_index = lax.axis_index("tp") * channels + jnp.arange(channels, dtype=jnp.int32)
    channel_group = channel_index * 4 // (channels * lax.axis_size("tp"))
    pooled = -floats
    for group_index, window in enumerate(WINDOWS):
        before = window // 2
        after_span = window - before
        upper_sum = jnp.pad(csum, ((0, 0), (0, after_span), (0, 0)), mode="edge")[
            :, after_span : after_span + SEQ
        ]
        lower_sum = jnp.pad(csum, ((0, 0), (before, 0), (0, 0)), mode="edge")[:, :SEQ]
        counts = (
            jnp.minimum(position + after_span, SEQ) - jnp.maximum(position - before, 0)
        ).astype(jnp.float32)
        window_mean = (upper_sum - lower_sum) / counts[None, :, None]
        select = (channel_group == group_index).astype(jnp.float32)
        pooled = pooled + window_mean * select
    return pooled.reshape(-1, channels).astype(jnp.bfloat16)


def body(
    stream,
    gain_first,
    gain_mixer,
    gain_second,
    gate_weight,
    gate_scale,
    up_weight,
    up_scale,
    down_weight,
    down_scale,
    pool_in_weight,
    pool_in_scale,
    pool_out_weight,
    pool_out_scale,
):
    hidden_width = gate_weight.shape[1]
    gate_in = jnp.concatenate([gate_weight, pool_in_weight], axis=1).astype(jnp.bfloat16)
    up_half = up_weight.astype(jnp.bfloat16)
    down_out = jnp.concatenate([down_weight, pool_out_weight], axis=0).astype(jnp.bfloat16)
    gate_in_whole = gather_fs(gate_in, 0)
    up_whole = gather_fs(up_half, 0)
    down_out_whole = gather_fs(down_out, 1)
    gate_whole, in_whole = gate_in_whole[:, :hidden_width], gate_in_whole[:, hidden_width:]
    down_whole, out_whole = down_out_whole[:hidden_width], down_out_whole[hidden_width:]

    def feed_forward(normed_rows):
        gate_sum = jnp.dot(normed_rows, gate_whole, preferred_element_type=jnp.float32) * gate_scale
        up_sum = jnp.dot(normed_rows, up_whole, preferred_element_type=jnp.float32) * up_scale
        hidden = (jax.nn.silu(gate_sum) * up_sum).astype(jnp.bfloat16)
        return jnp.dot(hidden, down_whole, preferred_element_type=jnp.float32)

    tp_count = lax.axis_size("tp")
    width = stream.shape[1]
    out_rows = jnp.concatenate(
        [out_whole[:, :width]]
        + [swap(out_whole[:, m * width : (m + 1) * width], "tp", m) for m in range(1, tp_count)],
        axis=0,
    )
    first_relative = relative_gain(gain_first)
    mixer_relative = relative_gain(gain_mixer)
    second_relative = relative_gain(gain_second)
    after_first = residual_add(stream, feed_forward(normed(stream, first_relative)), down_scale, 0.5)
    mixer_normed = normed(after_first, mixer_relative)
    pool_input = (
        jnp.dot(mixer_normed, in_whole, preferred_element_type=jnp.float32) * pool_in_scale
    ).astype(jnp.bfloat16)
    pooled = pooling(pool_input)
    all_pooled = jnp.concatenate(spread_tp(pooled), axis=1)
    mixed = jnp.dot(all_pooled, out_rows, preferred_element_type=jnp.float32)
    after_mix = (after_first.astype(jnp.float32) + mixed * pool_out_scale).astype(jnp.bfloat16)
    return residual_add(after_mix, feed_forward(normed(after_mix, second_relative)), down_scale, 0.5)


def solution(mesh):
    placed = (
        P("fs", "tp"),
        P(),
        P(),
        P(),
        P("fs", "tp"),
        P("tp"),
        P("fs", "tp"),
        P("tp"),
        P("tp", "fs"),
        P("tp"),
        P("fs", "tp"),
        P("tp"),
        P("tp", "fs"),
        P("tp"),
    )
    return jax.shard_map(body, mesh=mesh, in_specs=placed, out_specs=P("fs", "tp"), check_vma=False)
```
